128 devices in a mesh: ep: 32 (over z, y, core), tp: 4 (over x).
Axes of the slice: x: 4, y: 4, z: 4, core: 2. Of those that a mesh axis runs over, the one named last changes fastest.
Arguments:
- queries: bfloat16 [32768, 1024], P('ep', 'tp'), may hold values from -6 to 6
- keys: bfloat16 [32768, 1024], P('ep', 'tp'), may hold values from -6 to 6
- values: bfloat16 [32768, 2048], P('ep', 'tp'), may hold values from -6 to 6
- log_input_gate: float32 [32768, 8], P('ep', 'tp'), may hold values from -6 to 103
- forget_preactivation: float32 [32768, 8], P('ep', 'tp'), may hold values from 0 to 16
- forget_offset: float32 [32768, 8], P('ep', 'tp'), may hold values from -0.7 to 0
- head_norm_scale: float32 [2048], P('tp'), may hold values from 0.1 to 1.9
- memory_output_weight: bfloat16 [2048, 4096], P('tp'), may hold values from -0.125 to 0.125
- second_micro_tokens: bfloat16 [16384, 4096], P('ep'), may hold values from -6 to 6
- expert_norm_scale: float32 [4096], replicated, may hold values from 0.1 to 1.9
- expert_choice_index: int32 [16384, 2], P('ep'), may hold values from 0 to 63, all different within a row; in each aligned block of 512 rows (0 to 511, 512 to 1023, ...) at most 24 rows name the same one
- group_likelihood: float32 [16384], P('ep'), may hold values from 0.2 to 1
- expert_raw_weight: float32 [16384, 2], P('ep'), may hold values from 0.1 to 1
- gate_weight: bfloat16 [64, 4096, 1024], P('ep', None, 'tp'), may hold values from -0.09375 to 0.09375
- up_weight: bfloat16 [64, 4096, 1024], P('ep', None, 'tp'), may hold values from -0.09375 to 0.09375
- down_weight: bfloat16 [64, 1024, 4096], P('ep', 'tp'), may hold values from -0.1875 to 0.1875
Outputs:
- mixed: bfloat16 [32768, 4096], P(('ep', 'tp'))
- routed: bfloat16 [16384, 4096], P('ep', 'tp')
The draws below stay inside these ranges and needn't reach their ends.
Inputs may be any that keep to these rules, and one draw needn't show every extreme that they name: `expert_choice_index`: each row names 2 different experts. Within the 512 rows of one index of ep (aligned blocks) no expert is named more than 24 times, and in some blocks one expert is named exactly 24 times.
All inputs are finite; a program needn't handle non-finite values.
Results may differ from the reference program's by a relative error of at most 0.012.
Values may be sent and summed in bfloat16 or wider, within the bound.
No kernel may reach another device: no remote copies, remote signals or barrier semaphores. Data moves between devices by JAX's collectives and lax.ppermute only.
A program may use at most 192 MiB of HBM per device.

```python
import math
import jax
import jax.numpy as jnp
import numpy as np
from jax import lax

D = 4096
HEADS = 8
QK = 128
VH = 256
FFE = 1024
TOPK = 2
BLOCK = 128
TA_DEV = 1024
TB_DEV = 512
EXPERTS = 64
TOKA = 32768
TOKB = 16384
CAP = 24
N_EP = 32
N_TP = 4


def draw_log_input_gate(key, part):
    key_one = jax.random.fold_in(key, 0)
    base = -1.5 + 1.5 * jax.random.truncated_normal(key_one, -3.0, 3.0, (TOKA, HEADS), jnp.float32)
    return base


def draw_forget_preactivation(key, part):
    key_one, key_two, key_three, key_four, key_five = jax.random.split(key, 5)
    slow_heads = jax.random.uniform(key_one, (HEADS,), jnp.float32) < 0.5
    jitter = 0.6 * jax.random.truncated_normal(key_four, -2.0, 2.0, (TOKA, HEADS), jnp.float32)
    slow_rate = 0.5 / TOKA * jnp.exp(jax.random.uniform(key_two, (HEADS,), jnp.float32, -0.5, 0.5))
    fast_rate = jnp.exp(jax.random.uniform(key_three, (HEADS,), jnp.float32, math.log(1.0 / 50.0), math.log(1.0 / 30.0)))
    head_rate = jnp.where(slow_heads, slow_rate, fast_rate)
    device_factor = jnp.exp(jax.random.uniform(key_five, (TOKA // TA_DEV, HEADS), jnp.float32, -math.log(2.0), math.log(2.0)))
    device_factor = jnp.repeat(device_factor, TA_DEV, axis=0)
    rate = head_rate[None, :] * device_factor * jnp.exp(jitter)
    return -jnp.log(jnp.expm1(rate))


def draw_forget_offset(key, part):
    key_one, key_two = jax.random.split(key, 2)
    spots = jax.random.randint(key_one, (4,), 0, TOKA)
    struck = jnp.any(jnp.arange(TOKA, dtype=jnp.int32)[:, None] == spots[None, :], axis=1)
    depth = jnp.log(jax.random.uniform(key_two, (TOKA, HEADS), jnp.float32, 0.5, 0.8))
    return jnp.where(struck[:, None], depth, 0.0)


def steps_of(stream_key, extent, shards, least, high):
    def one(dim, blocks):
        draws = jax.random.uniform(jax.random.fold_in(jax.random.fold_in(stream_key, 6), dim), (blocks,), jnp.float32, least / len(shards), high / len(shards))
        return jnp.repeat(jnp.exp(draws), extent[dim] // blocks).reshape((-1,) + (1,) * (len(extent) - dim - 1))

    gain = one(*shards[0])
    for cut in shards[1:]:
        gain = gain * one(*cut)
    return gain


def routed_block(rng, own, number, rows, count, top, most, lean):
    order = jax.random.permutation(rng, count)
    packed, ordinary = portions_of(count, rows * top, most, lean, True), portions_of(count, rows * top, most, lean, False)
    places = jnp.arange(count)

    def named(lengths, turn):
        used = int((lengths > 0).sum())
        fixed = max(1, used // 4)
        shifted = fixed + (places - fixed + turn * (used - fixed)) % max(1, count - fixed)
        return jnp.zeros((count,), jnp.int32).at[order[jnp.where(places < fixed, places, shifted)]].set(jnp.asarray(lengths, jnp.int32))

    lengths = jnp.where(number % 4 == 0, named(packed, number // 4), named(ordinary, number - number // 4 - 1))
    mixed = jax.random.permutation(jax.random.fold_in(own, 3), count)
    donor, sink = mixed[0:count // 2 * 2:2], mixed[1:count // 2 * 2:2]
    margin = jnp.minimum(lengths[donor] - 1, most - lengths[sink]) // 2
    margin = jnp.where((donor == order[0]) | (sink == order[0]) | (lengths[sink] == 0), 0, jnp.maximum(margin, 0))
    shifted = jax.random.randint(jax.random.fold_in(own, 4), (count // 2,), 0, 1 << 20) % (margin + 1)
    lengths = lengths.at[donor].add(-shifted).at[sink].add(shifted)
    members = jnp.searchsorted(jnp.cumsum(lengths), jnp.arange(rows * top), side="right").astype(jnp.int32)
    grid = members.reshape(top, rows).T
    grid = grid[jax.random.permutation(jax.random.fold_in(own, 1), rows)]
    turn = jax.random.randint(jax.random.fold_in(own, 2), (rows, 1), 0, top)
    return jnp.take_along_axis(grid, (jnp.arange(top)[None, :] + turn) % top, axis=1)


def portions_of(count, total, reach, lean, full):
    loads = [(1 << 20) // math.isqrt(standing ** lean) + 1 for standing in range(1, count + 1)]
    largest = reach if full else min(reach, max(-(-total // count), total * loads[0] // sum(loads)))
    least = 1 if total - largest >= count - 1 else 0
    holding, rest = [largest] + [least] * (count - 1), total - largest - least * (count - 1)
    while rest > 0:
        candidates = [i for i in range(1, count) if holding[i] < largest] or [i for i in range(1, count) if holding[i] < reach]
        whole, left = sum([loads[i] for i in candidates]), rest
        for i in candidates:
            extra = min(reach - holding[i], max(1, left * loads[i] // whole), rest)
            holding[i] = holding[i] + extra
            rest = rest - extra
    return np.array(holding)


def noise(own_key, shape, deviation, limit, cuts=(), held_as=jnp.bfloat16):
    entries = deviation * jax.random.normal(own_key, shape, jnp.float32)
    if cuts:
        entries = entries * steps_of(own_key, shape, cuts, -0.22, 0.18)
    return jnp.clip(entries, -limit, limit).astype(held_as)


def setup_inputs(seed: int = 0) -> dict:
    streams_of = jax.random.split(jax.random.key(seed), 17)
    queries = noise(streams_of[0], (TOKA, HEADS * QK), 1.0, 6.0, ((0, 32), (1, 4)))
    keys = noise(streams_of[1], (TOKA, HEADS * QK), 1.0, 6.0, ((0, 32), (1, 4)))
    values = noise(streams_of[2], (TOKA, HEADS * VH), 1.0, 6.0, ((0, 32), (1, 4)))
    log_input_gate = draw_log_input_gate(jax.random.fold_in(streams_of[16], 71), 0)
    forget_preactivation = draw_forget_preactivation(jax.random.fold_in(streams_of[16], 71), 0)
    forget_offset = draw_forget_offset(jax.random.fold_in(streams_of[16], 71), 0)
    head_norm_scale = jnp.clip(1.0 + 0.18 * jax.random.normal(streams_of[6], (HEADS * VH,), jnp.float32), 0.1, 1.9)
    memory_output_weight = noise(streams_of[7], (HEADS * VH, D), (HEADS * VH) ** -0.5, 0.125, ((0, 4),))
    second_micro_tokens = noise(streams_of[8], (TOKB, D), 1.0, 6.0, ((0, 32),))
    expert_norm_scale = jnp.clip(1.0 + 0.18 * jax.random.normal(streams_of[9], (D,), jnp.float32), 0.1, 1.9)
    expert_choice_index_keys = jax.random.split(jax.random.fold_in(streams_of[10], 1), TOKB // TB_DEV)
    expert_choice_index_turns = jax.random.permutation(jax.random.fold_in(streams_of[10], 3), TOKB // TB_DEV)
    expert_choice_index = jax.vmap(lambda own, number: routed_block(jax.random.fold_in(streams_of[10], 2), own, number, TB_DEV, EXPERTS, TOPK, CAP, 1))(expert_choice_index_keys, expert_choice_index_turns).reshape((TOKB, TOPK))
    group_likelihood = jnp.clip(0.2 + 0.8 * jax.random.uniform(streams_of[11], (TOKB,), jnp.float32) ** steps_of(streams_of[11], (TOKB,), ((0, 32),), -0.2, 0.2), 0.2, 1.0)
    expert_raw_weight = jnp.clip(jnp.exp(math.log(1.0) - 2.3025851 * jax.random.uniform(streams_of[12], (TOKB, TOPK), jnp.float32) ** steps_of(streams_of[12], (TOKB, TOPK), ((0, 32),), -0.2, 0.2)), 0.1, 1.0)
    gate_weight = noise(streams_of[13], (EXPERTS, D, FFE), D ** -0.5, 0.09375, ((0, 32), (2, 4)))
    up_weight = noise(streams_of[14], (EXPERTS, D, FFE), D ** -0.5, 0.09375, ((0, 32), (2, 4)))
    down_weight = noise(streams_of[15], (EXPERTS, FFE, D), FFE ** -0.5, 0.1875, ((0, 32), (1, 4)))
    return dict(queries=queries, keys=keys, values=values, log_input_gate=log_input_gate, forget_preactivation=forget_preactivation, forget_offset=forget_offset, head_norm_scale=head_norm_scale, memory_output_weight=memory_output_weight, second_micro_tokens=second_micro_tokens, expert_norm_scale=expert_norm_scale, expert_choice_index=expert_choice_index, group_likelihood=group_likelihood, expert_raw_weight=expert_raw_weight, gate_weight=gate_weight, up_weight=up_weight, down_weight=down_weight)


EPSILON = 1e-06
FLOOR_LOG = -1e+30
HIGHEST = lax.Precision.HIGHEST

def memory_block(carry, piece):
    memory, stable_old = carry
    query_block, key_block, value_block, in_gate, forget_log_factor = piece
    query_float = query_block.astype(jnp.float32)
    key_float = key_block.astype(jnp.float32)
    value_float = value_block.astype(jnp.float32)
    qk_scale = 1.0 / math.sqrt(QK)
    raw_scores = jnp.einsum('htd,hsd->hts', query_float, key_float, precision=HIGHEST) * qk_scale
    running = jnp.cumsum(forget_log_factor, axis=-1)
    totals = running[:, -1]
    causal = jnp.tril(jnp.ones((BLOCK, BLOCK), dtype=bool))
    log_weight = jnp.where(causal, running[:, :, None] - running[:, None, :] + in_gate[:, None, :], -jnp.inf)
    carried = running + stable_old[:, None]
    stable = jnp.maximum(carried, lax.optimization_barrier(jnp.max(log_weight, axis=-1)))
    inner = (raw_scores * jnp.exp(log_weight - stable[..., None])).astype(jnp.bfloat16)
    inner = lax.optimization_barrier(inner).astype(jnp.float32)
    outer = jnp.exp(carried - stable)
    memory_half = lax.optimization_barrier(memory.astype(jnp.bfloat16)).astype(jnp.float32)
    state = outer[..., None] * jnp.einsum('htd,hde->hte', query_float, memory_half, precision=HIGHEST)
    state = state + jnp.einsum('hts,hse->hte', inner, value_float, precision=HIGHEST)
    to_end = totals[:, None] - running + in_gate
    block_peak = lax.optimization_barrier(jnp.max(to_end, axis=-1))
    scaled_keys = key_float * qk_scale
    weighted = (scaled_keys * jnp.exp(to_end - block_peak[:, None])[..., None]).astype(jnp.bfloat16)
    weighted = lax.optimization_barrier(weighted).astype(jnp.float32)
    update = jnp.einsum('hsd,hse->hde', weighted, value_float, precision=HIGHEST)
    stable_new = jnp.maximum(totals + stable_old, block_peak)
    memory = jnp.exp(totals + stable_old - stable_new)[:, None, None] * memory + jnp.exp(block_peak - stable_new)[:, None, None] * update
    return ((memory, stable_new), state)

def recurrence_baseline(queries, keys, values, log_input_gate, forget_preactivation, forget_offset, head_norm_scale, memory_output_weight):
    block_count = TOKA // BLOCK

    def to_blocks(array, width):
        return array.reshape(block_count, BLOCK, HEADS, width).transpose(0, 2, 1, 3)
    forget_log_factor = jax.nn.log_sigmoid(forget_preactivation) + forget_offset
    gate_blocks = log_input_gate.reshape(block_count, BLOCK, HEADS).transpose(0, 2, 1)
    forget_blocks = forget_log_factor.reshape(block_count, BLOCK, HEADS).transpose(0, 2, 1)
    start = (jnp.zeros((HEADS, QK, VH), jnp.float32), jnp.full((HEADS,), FLOOR_LOG, jnp.float32))
    unused, states = lax.scan(memory_block, start, (to_blocks(queries, QK), to_blocks(keys, QK), to_blocks(values, VH), gate_blocks, forget_blocks))
    states = states * lax.rsqrt(lax.optimization_barrier(jnp.mean(states * states, axis=-1, keepdims=True)) + EPSILON)
    hidden = states.transpose(0, 2, 1, 3).reshape(TOKA, HEADS * VH)
    hidden = (hidden * head_norm_scale).astype(jnp.bfloat16)
    group_width = HEADS // N_TP * VH
    total = jnp.zeros((TOKA, D), jnp.float32)
    for group in range(N_TP):
        part = jnp.dot(hidden[:, group * group_width:(group + 1) * group_width], memory_output_weight[group * group_width:(group + 1) * group_width], preferred_element_type=jnp.float32).astype(jnp.bfloat16)
        part = lax.optimization_barrier(part)
        total = total + part.astype(jnp.float32)
    return total.astype(jnp.bfloat16)

def expert_reference(second_micro_tokens, expert_norm_scale, expert_choice_index, group_likelihood, expert_raw_weight, gate_weight, up_weight, down_weight):
    token_float = second_micro_tokens.astype(jnp.float32)
    normed = token_float * lax.rsqrt(lax.optimization_barrier(jnp.mean(token_float * token_float, axis=-1, keepdims=True)) + EPSILON)
    normed = (normed * expert_norm_scale).astype(jnp.bfloat16)
    share = expert_raw_weight / lax.optimization_barrier(jnp.sum(expert_raw_weight, axis=1, keepdims=True))
    route_weight = group_likelihood[:, None] * share
    slot_limit = N_EP * CAP
    unit_width = FFE // N_TP

    def one_expert(total, expert):
        chosen = expert_choice_index == expert
        row_hit = jnp.any(chosen, axis=1)
        row_weight = lax.optimization_barrier(jnp.sum(jnp.where(chosen, route_weight, 0.0), axis=1))
        picked = jnp.nonzero(row_hit, size=slot_limit, fill_value=0)[0].astype(jnp.int32)
        live = (jnp.arange(slot_limit, dtype=jnp.int32) < jnp.sum(row_hit.astype(jnp.int32))).astype(jnp.float32)
        gathered = normed[picked]
        gate = jnp.dot(gathered, gate_weight[expert], preferred_element_type=jnp.float32)
        upward = jnp.dot(gathered, up_weight[expert], preferred_element_type=jnp.float32)
        hidden = (jax.nn.silu(gate) * upward).astype(jnp.bfloat16)
        down = down_weight[expert]
        summed = jnp.zeros((slot_limit, D), jnp.float32)
        for group in range(N_TP):
            part = jnp.dot(hidden[:, group * unit_width:(group + 1) * unit_width], down[group * unit_width:(group + 1) * unit_width], preferred_element_type=jnp.float32).astype(jnp.bfloat16)
            part = lax.optimization_barrier(part)
            summed = summed + part.astype(jnp.float32)
        expert_out = lax.optimization_barrier(summed.astype(jnp.bfloat16))
        contrib = expert_out.astype(jnp.float32) * (row_weight[picked] * live)[:, None]
        return (total.at[picked].add(contrib), None)
    total, unused = lax.scan(one_expert, jnp.zeros((TOKB, D), jnp.float32), jnp.arange(EXPERTS, dtype=jnp.int32))
    return total.astype(jnp.bfloat16)

def reference(queries, keys, values, log_input_gate, forget_preactivation, forget_offset, head_norm_scale, memory_output_weight, second_micro_tokens, expert_norm_scale, expert_choice_index, group_likelihood, expert_raw_weight, gate_weight, up_weight, down_weight):
    mixed = recurrence_baseline(queries, keys, values, log_input_gate, forget_preactivation, forget_offset, head_norm_scale, memory_output_weight)
    routed = expert_reference(second_micro_tokens, expert_norm_scale, expert_choice_index, group_likelihood, expert_raw_weight, gate_weight, up_weight, down_weight)
    return (mixed, routed)
```

```python
import functools
import math

import jax
import jax.numpy as jnp
from jax import lax
from jax.experimental import pallas as pl
from jax.experimental.pallas import tpu as pltpu
from jax.sharding import Mesh
from jax.sharding import PartitionSpec as P

BLOCK = 128
EP = ("ep_0", "ep_1", "ep_2")
EP_TP = ("ep_0", "ep_1", "ep_2", "tp")
EPSILON = 1e-06
FLOOR_LOG = -1e30
F32 = jnp.float32
BF16 = jnp.bfloat16
TURNED = 1024
TILE = 256


def shift_by(size, step):
    return [(i, (i + step) % size) for i in range(size)]


def gate_terms(log_input_gate, forget_preactivation, forget_offset):
    rows, heads = log_input_gate.shape
    blocks = rows // BLOCK
    logf = jax.nn.log_sigmoid(forget_preactivation) + forget_offset
    lower = jnp.tril(jnp.ones((BLOCK, BLOCK), F32))
    running = jnp.einsum(
        "ts,bsh->bth", lower, logf.reshape(blocks, BLOCK, heads), precision=lax.Precision.HIGHEST
    )
    totals = running[:, -1, :]
    a = log_input_gate.reshape(blocks, BLOCK, heads) - running
    return a, totals


def device_state(keys, values, a, totals):
    _, _, heads = a.shape
    rows = keys.shape[0]
    qk = keys.shape[1] // heads
    vh = values.shape[1] // heads
    after = jnp.flip(jnp.cumsum(jnp.flip(totals, 0), axis=0), 0)
    exponent = a + after[:, None, :]
    stable = jnp.max(exponent, axis=(0, 1))
    weight = jnp.exp(exponent - stable).reshape(rows, heads) * (1.0 / math.sqrt(qk))
    weighted = (keys.reshape(rows, heads, qk).astype(F32) * weight[..., None]).astype(BF16)
    memory = jnp.einsum(
        "shd,she->hde", weighted, values.reshape(rows, heads, vh), preferred_element_type=F32
    )
    return memory, stable, after[0]


def in_three(value):
    high = lax.reduce_precision(value, 8, 7)
    middle = lax.reduce_precision(value - high, 8, 7)
    low = value - high - middle
    return jnp.stack([high, middle, low]).astype(BF16)


def packed(state):
    memory, stable, total = state
    heads, qk, vh = memory.shape
    numbers = in_three(jnp.concatenate([stable, total])).reshape(1, -1)
    numbers = jnp.pad(numbers, ((0, 7), (0, vh - numbers.size)))
    return jnp.concatenate([memory.astype(BF16).reshape(heads * qk, vh), numbers])


def unpacked(message, heads):
    rows, vh = message.shape
    memory = message[: rows - 8].reshape(heads, (rows - 8) // heads, vh).astype(F32)
    numbers = message[rows - 8, : 6 * heads].astype(F32).reshape(3, 2, heads).sum(0)
    return memory, numbers[0], numbers[1]


def merged(states, order, limit):
    stables = jnp.stack([stable for _, stable, _ in states])
    totals = jnp.stack([total for _, _, total in states])
    later = (order[None, :] > order[:, None]) & (order[None, :] < limit)
    tail = jnp.sum(jnp.where(later[:, :, None], totals[None, :, :], 0.0), axis=1)
    used = (order < limit)[:, None]
    level = jnp.where(used, stables + tail, FLOOR_LOG)
    highest = jnp.max(level, axis=0)
    weight = jnp.where(used, jnp.exp(level - highest), 0.0)
    memory = sum(weight[k][:, None, None] * states[k][0] for k in range(len(states)))
    return memory, highest, jnp.sum(jnp.where(used, totals, 0.0), axis=0)


def state_before(state):
    heads = state[0].shape[0]
    before = None
    for axis in reversed(EP):
        members = lax.axis_size(axis)
        position = lax.axis_index(axis)
        message = packed(state)
        states = [state]
        for step in range(1, members):
            other = lax.ppermute(message, axis, shift_by(members, step))
            states.append(unpacked(other, heads))
        order = (position - jnp.arange(members)) % members
        inside = merged(states, order, position)
        if before is None:
            before = inside
        else:
            before = merged([inside, before], jnp.arange(2), 2)
        if axis != EP[0]:
            state = merged(states, order, members)
    return before[0], before[1]


def recurrence_body(tp_ref, q_ref, k_ref, v_ref, row_ref, col_ref, tot_ref, mem_ref, st_ref, gain_ref, out_ref):
    blocks = q_ref.shape[0] // BLOCK
    qk = mem_ref.shape[1]
    scale = 1.0 / math.sqrt(qk)
    heads = mem_ref.shape[0]
    vh = mem_ref.shape[2]
    t_index = lax.broadcasted_iota(jnp.int32, (BLOCK, BLOCK), 0)
    s_index = lax.broadcasted_iota(jnp.int32, (BLOCK, BLOCK), 1)
    causal = s_index <= t_index
    share = out_ref.shape[0] // 4
    per_share = share // BLOCK
    for h in range(heads):
        memory = mem_ref[h]
        stable = st_ref[h : h + 1, 0:1]
        gain = gain_ref[0:1, h * vh : (h + 1) * vh]
        for b in range(blocks):
            rows = pl.ds(b * BLOCK, BLOCK)
            q = q_ref[rows, h * qk : (h + 1) * qk]
            k = k_ref[rows, h * qk : (h + 1) * qk]
            v = v_ref[rows, h * vh : (h + 1) * vh]
            line = row_ref[b * heads + h : b * heads + h + 1, :]
            masked = jnp.where(causal, jnp.broadcast_to(line, (BLOCK, BLOCK)), -jnp.inf)
            high = jnp.maximum(jnp.max(masked, axis=1, keepdims=True), stable)
            scores = lax.dot_general(q, k, (((1,), (1,)), ((), ())), preferred_element_type=F32)
            inner = (scores * scale * jnp.exp(masked - high)).astype(BF16)
            outer = jnp.exp(stable - high)
            state = outer * jnp.dot(q, memory.astype(BF16), preferred_element_type=F32)
            state = state + jnp.dot(inner, v, preferred_element_type=F32)
            power = jnp.mean(state * state, axis=1, keepdims=True)
            place = (tp_ref[0] ^ (b // per_share)) * share + (b % per_share) * BLOCK
            out_ref[pl.ds(pl.multiple_of(place, BLOCK), BLOCK), h * vh : (h + 1) * vh] = (
                state * lax.rsqrt(power + EPSILON) * gain
            ).astype(BF16)
            if b + 1 < blocks:
                top = jnp.max(line, axis=1, keepdims=True)
                column = col_ref[rows, h : h + 1]
                wkey = (k.astype(F32) * scale * jnp.exp(column - top)).astype(BF16)
                update = lax.dot_general(
                    wkey, v, (((0,), (0,)), ((), ())), preferred_element_type=F32
                )
                higher = jnp.maximum(stable, top)
                memory = jnp.exp(stable - higher) * memory + jnp.exp(top - higher) * update
                stable = higher + tot_ref[b * heads + h : b * heads + h + 1, 0:1]


def recurrence_outputs(tp_index, queries, keys, values, a, totals, memory, stable, head_norm_scale):
    blocks, _, heads = a.shape
    rows = queries.shape[0]
    lines = a.transpose(0, 2, 1).reshape(blocks * heads, BLOCK)
    columns = a.reshape(rows, heads)
    tots = jnp.broadcast_to(totals.reshape(blocks * heads, 1), (blocks * heads, BLOCK))
    st = jnp.broadcast_to(stable[:, None], (heads, BLOCK))
    vmem = pl.BlockSpec(memory_space=pltpu.VMEM)
    return pl.pallas_call(
        recurrence_body,
        in_specs=[pl.BlockSpec(memory_space=pltpu.SMEM)] + [vmem] * 9,
        out_specs=vmem,
        out_shape=jax.ShapeDtypeStruct((rows, values.shape[1]), BF16),
        name="recurrence",
    )(tp_index, queries, keys, values, lines, columns, tots, memory, st, head_norm_scale[None, :])


def mixed_rows(hidden, weight):
    share = hidden.shape[0] // 4
    half = weight.shape[1] // 2
    left, right = weight[:, :half], weight[:, half:]
    flip_one = [(i, i ^ 1) for i in range(4)]
    flip_three = [(i, i ^ 3) for i in range(4)]

    def project(rows, columns):
        return jnp.dot(rows, columns, preferred_element_type=F32)

    send_left = project(hidden[share : 3 * share], left).astype(BF16)
    send_right = project(hidden[2 * share :], right).astype(BF16)
    got_left = lax.ppermute(send_left, "tp", flip_one)
    got_right = lax.ppermute(send_right, "tp", flip_three)
    keep = project(hidden[:share], weight)
    pass_left = (project(hidden[3 * share :], left) + got_left[share:].astype(F32)).astype(BF16)
    pass_right = (
        project(hidden[share : 2 * share], right) + got_right[:share].astype(F32)
    ).astype(BF16)
    last_left = lax.ppermute(pass_left, "tp", flip_three)
    last_right = lax.ppermute(pass_right, "tp", flip_one)
    sum_left = keep[:, :half] + got_left[:share].astype(F32) + last_left.astype(F32)
    sum_right = keep[:, half:] + got_right[share:].astype(F32) + last_right.astype(F32)
    return jnp.concatenate([sum_left.astype(BF16), sum_right.astype(BF16)], axis=1)


def dispatch_body(tp_ref, token_ref, gain_ref, lines_ref, out_ref, power_ref, select_ref, *, plan, tile):
    step = pl.program_id(0)
    slots = out_ref.shape[0]
    tokens = token_ref.shape[0]
    picks = lines_ref.shape[1]

    def set_select(expert):
        index = lax.broadcasted_iota(jnp.int32, (slots, tokens), 0)
        hit = index == lines_ref[expert, 0:1, :]
        for j in range(1, picks):
            hit = hit | (index == lines_ref[expert, j : j + 1, :])
        select_ref[...] = jnp.where(hit, 1.0, 0.0).astype(BF16)

    @pl.when(step == 0)
    def _():
        for r in range(0, tokens, 64):
            total = jnp.zeros((64, 128), F32)
            for c in range(0, token_ref.shape[1], 128):
                part = token_ref[r : r + 64, c : c + 128].astype(F32)
                total = total + part * part
            mean = jnp.sum(total, axis=1, keepdims=True) * (1.0 / token_ref.shape[1])
            power_ref[r : r + 64, :] = lax.rsqrt(mean + EPSILON)

    begin = 0
    for expert, count, first, per_tp in plan:

        @pl.when(step == begin)
        def _(expert=expert):
            set_select(expert)

        begin += count

    column = step
    begin = 0
    for expert, count, first, per_tp in plan:
        column = jnp.where(step >= begin, step - begin + first + per_tp * tp_ref[0], column)
        begin += count
    start = pl.multiple_of(column * tile, tile)
    normed = token_ref[:, pl.ds(start, tile)].astype(F32) * power_ref[...]
    normed = (normed * gain_ref[0:1, pl.ds(start, tile)]).astype(BF16)
    out_ref[...] = jnp.dot(select_ref[...], normed, preferred_element_type=F32).astype(BF16)


def dispatch_rows(tp_index, tokens, gain, lines, slots, plan, tile):
    rows, width = tokens.shape
    tiles = sum(entry[1] for entry in plan)
    return pl.pallas_call(
        functools.partial(dispatch_body, plan=plan, tile=tile),
        grid_spec=pltpu.PrefetchScalarGridSpec(
            num_scalar_prefetch=1,
            grid=(tiles,),
            in_specs=[
                pl.BlockSpec((rows, width), lambda i, tp: (0, 0)),
                pl.BlockSpec((1, width), lambda i, tp: (0, 0)),
                pl.BlockSpec(lines.shape, lambda i, tp: (0, 0, 0)),
            ],
            out_specs=pl.BlockSpec((slots, tile), lambda i, tp: (0, i)),
            scratch_shapes=[pltpu.VMEM((rows, 1), F32), pltpu.VMEM((slots, rows), BF16)],
        ),
        out_shape=jax.ShapeDtypeStruct((slots, tiles * tile), BF16),
        cost_estimate=pl.CostEstimate(
            flops=2 * slots * rows * tiles * tile,
            bytes_accessed=2 * (rows * width + slots * tiles * tile),
            transcendentals=rows,
        ),
        name="dispatch_rows",
    )(tp_index, tokens, gain[None, :], lines)


def hidden_body(tp_ref, main_ref, *refs):
    pieces, (gate_ref, up_ref, out_ref) = refs[:-3], refs[-3:]
    wide = main_ref.shape[1]
    main = main_ref[...]
    gate = jnp.dot(main, gate_ref[0, :wide, :], preferred_element_type=F32)
    upward = jnp.dot(main, up_ref[0, :wide, :], preferred_element_type=F32)
    for step, piece_ref in zip((0, 3, 1, 2), pieces):
        piece = piece_ref[...]
        size = piece.shape[1]
        start = pl.multiple_of(wide + ((tp_ref[0] + step) % 4) * size, 128)
        gate = gate + jnp.dot(piece, gate_ref[0, pl.ds(start, size), :], preferred_element_type=F32)
        upward = upward + jnp.dot(piece, up_ref[0, pl.ds(start, size), :], preferred_element_type=F32)
    out_ref[...] = (gate * jax.nn.sigmoid(gate) * upward).astype(BF16)


def hidden_units(tp_index, main, wide, pieces, gate_weight, up_weight, expert):
    rows = main.shape[0]
    tile = rows // 3
    _, width, units = gate_weight.shape
    turned = (width - wide) // 4

    def tiled(columns, at):
        return pl.BlockSpec((tile, columns), lambda i, tp: (i, at))

    whole = pl.BlockSpec((1, width, units), lambda i, tp: (expert, 0, 0))
    return pl.pallas_call(
        hidden_body,
        grid_spec=pltpu.PrefetchScalarGridSpec(
            num_scalar_prefetch=1,
            grid=(3,),
            in_specs=[tiled(wide, 0)] + [tiled(turned, at) for _, at in pieces] + [whole, whole],
            out_specs=pl.BlockSpec((tile, units), lambda i, tp: (i, 0)),
        ),
        out_shape=jax.ShapeDtypeStruct((rows, units), BF16),
        cost_estimate=pl.CostEstimate(
            flops=4 * rows * width * units,
            bytes_accessed=2 * (rows * width + 2 * width * units),
            transcendentals=rows * units,
        ),
        name="hidden_units",
    )(tp_index, main, *[array for array, _ in pieces], gate_weight, up_weight)


def down_body(tp_ref, *refs):
    out_ref = refs[-1]
    total = jnp.dot(refs[0][...], refs[4][0], preferred_element_type=F32)
    for k in range(1, 4):
        total = total + jnp.dot(refs[k][...], refs[4 + k][0], preferred_element_type=F32)
    out_ref[...] = total.astype(BF16)


def down_columns(tp_index, hiddens, down_weight, shares, expert):
    rows, units = hiddens[0].shape
    columns = shares[0].shape[2]
    tile = rows // 3
    line = pl.BlockSpec((tile, units), lambda i, tp: (i, 0))
    own = pl.BlockSpec((1, units, columns), lambda i, tp: (expert, 0, tp[0]))
    other = pl.BlockSpec((1, units, columns), lambda i, tp: (expert, 0, 0))
    return pl.pallas_call(
        down_body,
        grid_spec=pltpu.PrefetchScalarGridSpec(
            num_scalar_prefetch=1,
            grid=(3,),
            in_specs=[line] * 4 + [own] + [other] * 3,
            out_specs=pl.BlockSpec((tile, columns), lambda i, tp: (i, 0)),
        ),
        out_shape=jax.ShapeDtypeStruct((rows, columns), BF16),
        cost_estimate=pl.CostEstimate(
            flops=8 * rows * units * columns,
            bytes_accessed=2 * (4 * rows * units + 4 * units * columns + rows * columns),
            transcendentals=0,
        ),
        name="down_columns",
    )(tp_index, *hiddens, down_weight, *shares)


def route(expert_choice_index, group_likelihood, expert_raw_weight, expert_count):
    share = expert_raw_weight / jnp.sum(expert_raw_weight, axis=1, keepdims=True)
    weight = group_likelihood[:, None] * share
    tokens, _ = expert_choice_index.shape
    experts = jnp.arange(expert_count, dtype=jnp.int32)
    hit = jnp.any(expert_choice_index[:, :, None] == experts, axis=1)
    earlier = jnp.tril(jnp.ones((tokens, tokens), BF16), -1)
    count = jnp.dot(earlier, hit.astype(BF16), preferred_element_type=F32)
    rank = jnp.sum(
        jnp.where(expert_choice_index[:, :, None] == experts, count[:, None, :], 0.0), axis=2
    ).astype(jnp.int32)
    return weight, rank


def both_halves(
    queries,
    keys,
    values,
    log_input_gate,
    forget_preactivation,
    forget_offset,
    head_norm_scale,
    memory_output_weight,
    second_micro_tokens,
    expert_norm_scale,
    expert_choice_index,
    group_likelihood,
    expert_raw_weight,
    gate_weight,
    up_weight,
    down_weight,
):
    ep_size = lax.axis_size(EP)
    tp_size = lax.axis_size("tp")
    tp_index = lax.axis_index("tp")
    tokens, width = second_micro_tokens.shape
    picks = expert_choice_index.shape[1]
    local_experts = gate_weight.shape[0]
    expert_count = local_experts * ep_size
    capacity = tp_size * max(1, 3 * picks * tokens // (2 * expert_count * tp_size))
    slots = ep_size * capacity
    columns = width // tp_size

    tp_scalar = tp_index.astype(jnp.int32).reshape(1)
    wide = width - TURNED
    turned = TURNED // tp_size

    a, totals = gate_terms(log_input_gate, forget_preactivation, forget_offset)
    memory, stable = state_before(device_state(keys, values, a, totals))

    weight, rank = route(expert_choice_index, group_likelihood, expert_raw_weight, expert_count)
    owner = expert_choice_index // local_experts
    local = expert_choice_index % local_experts
    slot = owner * capacity + rank
    slot_index = jnp.arange(slots, dtype=jnp.int32)
    places = [jnp.where(local == e, slot, -1) for e in range(local_experts)]
    lines = jnp.stack([place.T for place in places])

    whole_tiles, wide_tiles, turned_tiles = width // TILE, wide // TILE, turned // TILE
    plans = [[(0, whole_tiles, 0, 0)], [(1, wide_tiles, 0, 0)]]
    if turned:
        plans[0].append((1, turned_tiles, wide_tiles, turned_tiles))
    arrived = []
    for e in range(local_experts):
        outgoing = dispatch_rows(
            tp_scalar, second_micro_tokens, expert_norm_scale, lines, slots, plans[e], TILE
        )
        outgoing = outgoing.reshape(ep_size, capacity, outgoing.shape[1])
        got = lax.all_to_all(outgoing, EP, split_axis=0, concat_axis=0, tiled=True)
        arrived.append(got.reshape(slots, got.shape[2]))

    pieces = [[], []]
    if turned:
        own = arrived[0][:, width:]
        left = lax.ppermute(own, "tp", shift_by(4, 1))
        right = lax.ppermute(own, "tp", shift_by(4, -1))
        far = lax.ppermute(own, "tp", shift_by(4, 2))
        pieces[1] = [(arrived[0], width // turned), (left, 0), (right, 0), (far, 0)]

    shares = []
    for step in range(1, tp_size):
        piece = lax.dynamic_slice_in_dim(
            down_weight, ((tp_index + step) % tp_size) * columns, columns, 2
        )
        shares.append(lax.ppermute(piece, "tp", shift_by(tp_size, step)))

    hidden_a = recurrence_outputs(
        tp_scalar, queries, keys, values, a, totals, memory, stable, head_norm_scale
    )
    mixed = mixed_rows(hidden_a, memory_output_weight)

    combined = jnp.zeros((tokens, columns), F32)
    for e in range(local_experts):
        hidden = hidden_units(
            tp_scalar, arrived[e], wide if e else width, pieces[e], gate_weight, up_weight, e
        )
        hiddens = [hidden]
        for step in range(1, tp_size):
            hiddens.append(lax.ppermute(hidden, "tp", shift_by(tp_size, step)))
        finished = down_columns(tp_scalar, hiddens, down_weight, shares, e)
        finished = finished.reshape(ep_size, capacity, columns)
        returned = lax.all_to_all(finished, EP, split_axis=0, concat_axis=0, tiled=True)
        returned = returned.reshape(slots, columns)
        place = jnp.where(
            places[e][:, :, None] == slot_index[None, None, :], weight[:, :, None], 0.0
        ).sum(axis=1)
        high = lax.reduce_precision(place, 8, 7)
        low = (place - high).astype(BF16)
        high = high.astype(BF16)
        combined = combined + jnp.dot(high, returned, preferred_element_type=F32)
        combined = combined + jnp.dot(low, returned, preferred_element_type=F32)
    return mixed, combined.astype(BF16)


def solution(mesh):
    split = Mesh(mesh.devices.reshape(4, 4, 2, mesh.shape["tp"]), EP_TP)
    placed = (
        P(EP, "tp"),
        P(EP, "tp"),
        P(EP, "tp"),
        P(EP, "tp"),
        P(EP, "tp"),
        P(EP, "tp"),
        P("tp"),
        P("tp", None),
        P(EP, None),
        P(),
        P(EP, None),
        P(EP),
        P(EP, None),
        P(EP, None, "tp"),
        P(EP, None, "tp"),
        P(EP, "tp", None),
    )
    return jax.shard_map(
        both_halves,
        mesh=split,
        in_specs=placed,
        out_specs=(P(EP_TP, None), P(EP, "tp")),
        check_vma=False,
    )
```
